32 devices in a mesh: grp: 2 (over y), ep: 4 (over z), tp: 4 (over x, core).
Axes of the slice: x: 2, y: 2, z: 4, core: 2. Of those that a mesh axis runs over, the one named last changes fastest.
Arguments:
- tokens: bfloat16 [2048, 2048], P(('grp', 'ep')), parts along dimension 0, may hold values from -6 to 6
- norm_gain: float32 [2048], replicated, may hold values from 0.1 to 1.9
- routing: int32 [2048, 2], P(('grp', 'ep')), parts along dimension 0, may hold values from 0 to 3, all different within a row; in each aligned block of 256 rows (0 to 255, 256 to 511, ...) at most 192 rows name the same one
- gate_weights: float32 [2048, 2], P(('grp', 'ep')), parts along dimension 0, may hold values from 0.2 to 2
- expert_gate: bfloat16 [4, 2048, 1024], P('ep', None, 'tp'), may hold values from -0.125 to 0.125
- expert_up: bfloat16 [4, 2048, 1024], P('ep', None, 'tp'), may hold values from -0.125 to 0.125
- expert_down: bfloat16 [4, 1024, 2048], P('ep', 'tp'), may hold values from -0.1875 to 0.1875
- shared_gate: bfloat16 [2048, 512], P(None, 'tp'), may hold values from -0.125 to 0.125
- shared_up: bfloat16 [2048, 512], P(None, 'tp'), may hold values from -0.125 to 0.125
- shared_down: bfloat16 [512, 2048], P('tp'), may hold values from -0.25 to 0.25
Outputs:
- mixed: bfloat16 [2048, 2048], P(('grp', 'ep'), 'tp'), parts along dimension 0
The draws below stay inside these ranges and needn't reach their ends.
There are 2 independent parts, one for each index of `grp`. The reference program is written for one: setup_inputs(seed, part) draws one part's arguments, and reference() takes and returns one part's arrays. A program takes and returns all parts, laid end to end along the dimension named above; an argument that names none is the same for every part. Nothing has to cross between parts.
Inputs may be any that keep to these rules, and one draw needn't show every extreme that they name: `routing`: each row names 2 different experts. Within each aligned block of 256 rows no expert is named by more than 192 rows, and in every draw some block has an expert named by exactly 192 rows.
All inputs are finite; a program needn't handle non-finite values.
Results may differ from the reference program's by a relative error of at most 0.012.
Values may be sent and summed in bfloat16 or wider, within the bound.
A program may use at most 64 MiB of HBM per device.

```python
import math
import jax
import jax.numpy as jnp
import numpy as np
from jax import lax

D = 2048
FFE = 1024
FFS = 512
TOP_K = 2
TOK_DEV = 256
EXPERTS = 4
CAP = 192
TOKENS = 1024
N_EP = 4
N_TP = 4


def level_of(rng, extent, pieces, smallest, top_value):
    def one(axis_at, shards_of):
        heights = jax.random.uniform(jax.random.fold_in(jax.random.fold_in(rng, 6), axis_at), (shards_of,), jnp.float32, smallest / len(pieces), top_value / len(pieces))
        return jnp.repeat(jnp.exp(heights), extent[axis_at] // shards_of).reshape((-1,) + (1,) * (len(extent) - axis_at - 1))

    factor_of = one(*pieces[0])
    for cut in pieces[1:]:
        factor_of = factor_of * one(*cut)
    return factor_of


def routed_block(stream_key, own, number, rows, count, top, most, slope):
    ranking = jax.random.permutation(stream_key, count)
    heavy_load, ordinary = shares(count, rows * top, most, slope, True), shares(count, rows * top, most, slope, False)
    places = jnp.arange(count)

    def named(tallies, rotation):
        used = int((tallies > 0).sum())
        fixed = max(1, used // 4)
        shifted = fixed + (places - fixed + rotation * (used - fixed)) % max(1, count - fixed)
        return jnp.zeros((count,), jnp.int32).at[ranking[jnp.where(places < fixed, places, shifted)]].set(jnp.asarray(tallies, jnp.int32))

    tallies = jnp.where(number % 4 == 0, named(heavy_load, number // 4), named(ordinary, number - number // 4 - 1))
    mixed = jax.random.permutation(jax.random.fold_in(own, 3), count)
    giver, taker = mixed[0:count // 2 * 2:2], mixed[1:count // 2 * 2:2]
    room = jnp.minimum(tallies[giver] - 1, most - tallies[taker]) // 2
    room = jnp.where((giver == ranking[0]) | (taker == ranking[0]) | (tallies[taker] == 0), 0, jnp.maximum(room, 0))
    shifted = jax.random.randint(jax.random.fold_in(own, 4), (count // 2,), 0, 1 << 20) % (room + 1)
    tallies = tallies.at[giver].add(-shifted).at[taker].add(shifted)
    items = jnp.searchsorted(jnp.cumsum(tallies), jnp.arange(rows * top), side="right").astype(jnp.int32)
    grid = items.reshape(top, rows).T
    grid = grid[jax.random.permutation(jax.random.fold_in(own, 1), rows)]
    rotation = jax.random.randint(jax.random.fold_in(own, 2), (rows, 1), 0, top)
    return jnp.take_along_axis(grid, (jnp.arange(top)[None, :] + rotation) % top, axis=1)


def shares(number_of, total, limit, skew, full):
    portions = [(1 << 20) // math.isqrt(grade ** skew) + 1 for grade in range(1, number_of + 1)]
    largest = limit if full else min(limit, max(-(-total // number_of), total * portions[0] // sum(portions)))
    least = 1 if total - largest >= number_of - 1 else 0
    holding, rest = [largest] + [least] * (number_of - 1), total - largest - least * (number_of - 1)
    while rest > 0:
        free = [i for i in range(1, number_of) if holding[i] < largest] or [i for i in range(1, number_of) if holding[i] < limit]
        mass, remaining = sum([portions[i] for i in free]), rest
        for i in free:
            addition = min(limit - holding[i], max(1, remaining * portions[i] // mass), rest)
            holding[i] = holding[i] + addition
            rest = rest - addition
    return np.array(holding)


def bell_draw(own_key, dims, scale, reach, cuts=(), held_as=jnp.bfloat16):
    gain = level_of(own_key, dims, cuts, -0.22, 0.18) if cuts else 1.0
    result = jax.random.normal(own_key, dims, jnp.float32) * scale * gain
    return jnp.minimum(jnp.maximum(result, -reach), reach).astype(held_as)


def setup_inputs(seed: int = 0, part: int = 0) -> dict:
    streams_of = jax.random.split(jax.random.key(seed), 11)
    part_keys = jax.random.split(jax.random.fold_in(streams_of[10], part), 11)
    tokens = bell_draw(part_keys[0], (TOKENS, D), 1.0, 6.0, ((0, 4),))
    norm_gain = jnp.clip(1.0 + 0.18 * jax.random.normal(streams_of[1], (D,), jnp.float32), 0.1, 1.9)
    routing_keys = jax.random.split(jax.random.fold_in(part_keys[2], 1), TOKENS // TOK_DEV)
    routing_turns = jax.random.permutation(jax.random.fold_in(part_keys[2], 3), TOKENS // TOK_DEV)
    routing = jax.vmap(lambda own, number: routed_block(jax.random.fold_in(part_keys[2], 2), own, number, TOK_DEV, EXPERTS, TOP_K, CAP, 2))(routing_keys, routing_turns).reshape((TOKENS, TOP_K))
    gate_weights = jnp.clip(jnp.exp(math.log(2.0) - 2.3025851 * jax.random.uniform(part_keys[3], (TOKENS, TOP_K), jnp.float32) ** level_of(part_keys[3], (TOKENS, TOP_K), ((0, 4),), -0.2, 0.2)), 0.2, 2.0)
    expert_gate = bell_draw(streams_of[4], (EXPERTS, D, FFE), D ** -0.5, 0.125, ((0, 4), (2, 4)))
    expert_up = bell_draw(streams_of[5], (EXPERTS, D, FFE), D ** -0.5, 0.125, ((0, 4), (2, 4)))
    expert_down = bell_draw(streams_of[6], (EXPERTS, FFE, D), FFE ** -0.5, 0.1875, ((0, 4), (1, 4)))
    shared_gate = bell_draw(streams_of[7], (D, FFS), D ** -0.5, 0.125, ((1, 4),))
    shared_up = bell_draw(streams_of[8], (D, FFS), D ** -0.5, 0.125, ((1, 4),))
    shared_down = bell_draw(streams_of[9], (FFS, D), FFS ** -0.5, 0.25, ((0, 4),))
    return dict(tokens=tokens, norm_gain=norm_gain, routing=routing, gate_weights=gate_weights, expert_gate=expert_gate, expert_up=expert_up, expert_down=expert_down, shared_gate=shared_gate, shared_up=shared_up, shared_down=shared_down)


def norm_rows(tokens, norm_gain):
    values = tokens.astype(jnp.float32)
    scale = lax.rsqrt(lax.optimization_barrier(jnp.mean(values * values, axis=-1, keepdims=True)) + 1e-06)
    return (values * scale * norm_gain).astype(jnp.bfloat16)

def grouped_down(hidden, down):
    width = hidden.shape[1] // N_TP
    total = jnp.zeros((hidden.shape[0], down.shape[1]), jnp.float32)
    for group in range(N_TP):
        partial_sum = jnp.dot(hidden[:, group * width:(group + 1) * width], down[group * width:(group + 1) * width], preferred_element_type=jnp.float32)
        total = total + partial_sum.astype(jnp.bfloat16).astype(jnp.float32)
    return total

def swiglu_hidden(rows, w_gate, w_up):
    gate = jnp.dot(rows, w_gate, preferred_element_type=jnp.float32)
    up = jnp.dot(rows, w_up, preferred_element_type=jnp.float32)
    return (jax.nn.silu(gate) * up).astype(jnp.bfloat16)

def reference(tokens, norm_gain, routing, gate_weights, expert_gate, expert_up, expert_down, shared_gate, shared_up, shared_down):
    normed = norm_rows(tokens, norm_gain)
    assign = TOK_DEV * TOP_K
    blocks = routing.reshape(N_EP, assign).astype(jnp.int32)
    onehot = (blocks[:, :, None] == jnp.arange(EXPERTS, dtype=jnp.int32)[None, None, :]).astype(jnp.int32)
    slot = lax.optimization_barrier(jnp.sum(jnp.cumsum(onehot, axis=1) * onehot, axis=2)).astype(jnp.int32) - 1
    dest = blocks * CAP + slot
    owner = (jnp.arange(N_EP, dtype=jnp.int32)[:, None] * TOK_DEV + jnp.arange(assign, dtype=jnp.int32)[None, :] // TOP_K).astype(jnp.int32)

    def fill_table(where, who):
        return jnp.full((EXPERTS * CAP,), TOKENS, jnp.int32).at[where].set(who)
    table = jax.vmap(fill_table)(dest, owner)
    table = table.reshape(N_EP, EXPERTS, CAP).transpose(1, 0, 2).reshape(EXPERTS, N_EP * CAP)
    padded = jnp.concatenate([normed, jnp.zeros((1, D), jnp.bfloat16)], axis=0)

    def one_expert(items):
        index, w_gate, w_up, w_down = items
        hidden = swiglu_hidden(padded[index], w_gate, w_up)
        return grouped_down(hidden, w_down).astype(jnp.bfloat16)
    outputs = lax.map(one_expert, (table, expert_gate, expert_up, expert_down))
    flat_index = blocks * (N_EP * CAP) + jnp.arange(N_EP, dtype=jnp.int32)[:, None] * CAP + slot
    picked = outputs.reshape(EXPERTS * N_EP * CAP, D)[flat_index.reshape(TOKENS * TOP_K)]
    picked = picked.astype(jnp.float32).reshape(TOKENS, TOP_K, D)
    routed = lax.optimization_barrier(jnp.sum(picked * gate_weights[:, :, None], axis=1))
    shared_out = grouped_down(swiglu_hidden(normed, shared_gate, shared_up), shared_down)
    return (routed + shared_out).astype(jnp.bfloat16)
```

```python
import jax
import jax.numpy as jnp
from jax import lax
from jax.experimental import pallas as pl
from jax.experimental.pallas import tpu as pltpu
from jax.sharding import PartitionSpec as P


def norm_rows(tokens, norm_gain):
    values = tokens.astype(jnp.float32)
    scale = lax.rsqrt(jnp.mean(values * values, axis=-1, keepdims=True) + 1e-06)
    return (values * scale * norm_gain).astype(jnp.bfloat16)


def body(
    tokens,
    norm_gain,
    routing,
    gate_weights,
    expert_gate,
    expert_up,
    expert_down,
    shared_gate,
    shared_up,
    shared_down,
):
    ep_count = lax.axis_size("ep")
    tp_count = lax.axis_size("tp")
    tok_rows, width = tokens.shape
    top = routing.shape[1]
    local_experts = expert_gate.shape[0]
    experts = ep_count * local_experts
    capacity = max(2, 3 * tok_rows * top // (2 * experts))
    quarter = width // tp_count
    arrived_rows = ep_count * capacity
    normed = norm_rows(tokens, norm_gain)
    flat_experts = routing.reshape(-1)
    assign = flat_experts.shape[0]
    onehot = (flat_experts[:, None] == jnp.arange(experts, dtype=jnp.int32)[None, :]).astype(
        jnp.float32
    )
    lower = (jnp.arange(assign)[:, None] >= jnp.arange(assign)[None, :]).astype(jnp.float32)
    running = jnp.dot(lower, onehot, precision=lax.Precision.HIGHEST)
    slot = (jnp.sum(running * onehot, axis=1) - 1.0).astype(jnp.int32)
    dest = flat_experts * capacity + slot
    owner = jnp.arange(assign, dtype=jnp.int32) // top
    slot_token = jnp.full((experts * capacity,), tok_rows, jnp.int32).at[dest].set(owner)
    padded = jnp.concatenate([normed, jnp.zeros((1, width), jnp.bfloat16)], axis=0)
    outgoing = padded[slot_token].reshape(experts, capacity, width)
    position = lax.axis_index("tp")
    own_columns = lax.dynamic_slice_in_dim(outgoing, position * quarter, quarter, 2)
    arrived = lax.all_to_all(own_columns, "ep", split_axis=0, concat_axis=0, tiled=True)
    piece = lax.all_gather(arrived, "tp", axis=2, tiled=True)
    count = piece.shape[2]
    piece = piece.reshape(ep_count, local_experts, capacity, count)
    local = 0
    rows = piece[:, local].reshape(arrived_rows, count)
    gate_rows = expert_gate[local]
    up_rows = expert_up[local]
    gate_list = [jnp.dot(rows, gate_rows, preferred_element_type=jnp.float32)]
    up_list = [jnp.dot(rows, up_rows, preferred_element_type=jnp.float32)]
    gate_all = jnp.stack(gate_list)
    up_all = jnp.stack(up_list)
    local = 0
    hidden = (jax.nn.silu(gate_all[local]) * up_all[local]).astype(jnp.bfloat16)
    term = jnp.dot(hidden, expert_down[local], preferred_element_type=jnp.float32)
    routed_list = [term.reshape(ep_count, capacity, width)]
    routed_terms = jnp.stack(routed_list, axis=1).reshape(experts * capacity, width)
    shared_gate_rows = jnp.dot(normed, shared_gate, preferred_element_type=jnp.float32)
    shared_up_rows = jnp.dot(normed, shared_up, preferred_element_type=jnp.float32)
    shared_hidden = (jax.nn.silu(shared_gate_rows) * shared_up_rows).astype(jnp.bfloat16)
    shared_term = jnp.dot(shared_hidden, shared_down, preferred_element_type=jnp.float32)
    routed_sum, shared_sum = (
        lax.psum_scatter(
            routed_terms.astype(jnp.bfloat16), "tp", scatter_dimension=1, tiled=True
        ).astype(jnp.float32),
        lax.psum_scatter(
            shared_term.astype(jnp.bfloat16), "tp", scatter_dimension=1, tiled=True
        ).astype(jnp.float32),
    )
    expert_out = routed_sum.astype(jnp.bfloat16).reshape(experts, capacity, quarter)
    returned = lax.all_to_all(expert_out, "ep", split_axis=0, concat_axis=0, tiled=True)
    picked = returned.reshape(experts * capacity, quarter)[dest]
    picked = picked.astype(jnp.float32).reshape(tok_rows, top, quarter)
    routed = jnp.sum(picked * gate_weights[:, :, None], axis=1)
    return (routed + shared_sum).astype(jnp.bfloat16)


MESH = pl.DeviceIdType.MESH


def silu(v):
    return v / (1.0 + jnp.exp(-v))


def dot32(a, b):
    return jnp.dot(a, b, preferred_element_type=jnp.float32)


OUTER = (
    "sp1", "own", "ap1", "pair", "s20", "s21", "s31", "wt", "ap0", "s30",
    "cp", "aF1", "sr0", "aF0", "gp0", "sp0", "aN0", "aN1", "cF", "gp1",
    "cN", "gF0", "gF1", "gN0", "gN1",
)
INNER = (
    "sp1", "s31", "s30", "own", "sp0", "aN1", "aN0", "ap1", "sr0", "wt",
    "aF0", "aF1", "cN", "s20", "s21", "cF", "pair", "gN0", "gN1", "ap0",
    "gF0", "gF1", "cp", "gp0", "gp1",
)
REDUNDANT = 1
LAST = (2, 3, 1)


def make_kernel(half, redundant):
    def kernel(
        tok_ref, gain_ref, routing_ref, gw_ref, wg_hbm, wu_hbm, wd_hbm, sg_hbm, su_hbm, sd_hbm,
        out_ref,
        wg, wu, wd, sg, su, sd, nq, pick, place, weight_ref,
        zsend, zred, xq, esend, erecv, own_keep, own_send, own_recv,
        fsend, frecv, keep, gsend, grecv,
        wsem, ws, wr, zs, zr, rs, rr, xs, xr, es, er, ps, pr, fs, fr, gs, gr,
    ):
        e = lax.axis_index("ep")
        t = lax.axis_index("tp")
        x = t // 2
        c = t % 2
        core = {"tp": t ^ 1}
        across = {"tp": t ^ 2}
        rows, width = tok_ref.shape
        quarter = width // 4

        barrier = pltpu.get_barrier_semaphore()
        for k in (1, 2, 3):
            for d in range(2):
                pl.semaphore_signal(
                    barrier, inc=1, device_id={"ep": e ^ k, "tp": 2 * x + d}, device_id_type=MESH
                )
        pl.semaphore_signal(barrier, inc=1, device_id=core, device_id_type=MESH)
        pl.semaphore_signal(barrier, inc=1, device_id=across, device_id_type=MESH)

        def meet():
            pl.semaphore_wait(barrier, 8)

        loads = [
            pltpu.make_async_copy(a, b, wsem.at[i])
            for i, (a, b) in enumerate(
                [
                    (wg_hbm, wg.at[c]), (wu_hbm, wu.at[c]), (wd_hbm, wd.at[c]),
                    (sg_hbm, sg), (su_hbm, su), (sd_hbm, sd),
                ]
            )
        ]
        for load in loads:
            load.start()

        values = tok_ref[...].astype(jnp.float32)
        scale = lax.rsqrt(jnp.mean(values * values, axis=-1, keepdims=True) + 1e-06)
        normed = (values * scale * gain_ref[...]).astype(jnp.bfloat16)
        for q in range(4):
            nq[q] = normed[:, q * quarter:(q + 1) * quarter]

        named = lax.broadcasted_iota(jnp.int32, (16, rows), 0) ^ e
        hit = jnp.zeros((16, rows), jnp.float32)
        weight = jnp.zeros((16, rows), jnp.float32)
        for j in range(routing_ref.shape[0]):
            same = routing_ref[j:j + 1, :] == named
            hit = hit + jnp.where(same, 1.0, 0.0)
            weight = weight + jnp.where(same, gw_ref[j:j + 1, :], 0.0)
        earlier = (
            lax.broadcasted_iota(jnp.int32, (rows, rows), 0)
            < lax.broadcasted_iota(jnp.int32, (rows, rows), 1)
        )
        earlier = jnp.where(earlier, 1.0, 0.0).astype(jnp.bfloat16)
        rank = dot32(hit.astype(jnp.bfloat16), earlier)
        rank = jnp.where(hit > 0.5, rank, -1.0)
        down = lax.broadcasted_iota(jnp.int32, (half, rows), 0).astype(jnp.float32)
        for k in (1, 2, 3):
            for d in range(2):
                pick[k - 1, d] = jnp.where(
                    rank[k:k + 1, :] == down + float(d * half), 1.0, 0.0
                ).astype(jnp.bfloat16)
        side = lax.broadcasted_iota(jnp.int32, (rows, half), 1).astype(jnp.float32)

        def finish_tables():
            weight_ref[...] = weight.T
            turned = rank.T
            for k in (1, 2, 3):
                for d in range(2):
                    place[k - 1, d] = jnp.where(
                        turned[:, k:k + 1] == side + float(d * half), 1.0, 0.0
                    ).astype(jnp.bfloat16)

        def remote(src, dst, send, recv, to):
            return pltpu.make_async_remote_copy(
                src_ref=src, dst_ref=dst, send_sem=send, recv_sem=recv,
                device_id=to, device_id_type=MESH,
            )

        def weight_copy(i):
            ref = (wg, wu, wd)[i].at[c]
            return remote(ref, ref, ws.at[i], wr.at[i], core)

        def zcopy(k, j):
            return remote(
                zsend.at[k - 1, j], xq.at[k - 1, 2 * x + j],
                zs.at[k - 1, j], zr.at[k - 1, j], {"ep": e ^ k},
            )

        def rcopy(j):
            return remote(
                zred.at[j], xq.at[0, 2 * (1 - x) + j], rs.at[j], rr.at[j], {"ep": e ^ 1}
            )

        def xcopy(k, j):
            mine = xq.at[k - 1, 2 * x + j]
            return remote(mine, mine, xs.at[k - 1, j], xr.at[k - 1, j], across)

        def ecopy():
            return remote(esend, erecv, es.at[0], er.at[0], core)

        def pcopy():
            return remote(own_send, own_recv, ps.at[0], pr.at[0], across)

        def fcopy(k, j):
            return remote(
                fsend.at[k - 1, j], frecv.at[k - 1, j],
                fs.at[k - 1, j], fr.at[k - 1, j], across,
            )

        def gcopy(k, j, d):
            return remote(
                gsend.at[k - 1, j], grecv.at[k - 1, d],
                gs.at[k - 1, j], gr.at[k - 1, d], {"ep": e ^ k, "tp": 2 * x + j},
            )

        def columns(q):
            return pl.ds(pl.multiple_of(q * quarter, quarter), quarter)

        def hidden_of(pieces, w_gate, w_up):
            gate, up = 0.0, 0.0
            for q in range(4):
                part = slice(q * quarter, (q + 1) * quarter)
                gate = gate + dot32(pieces(q), w_gate[part, :])
                up = up + dot32(pieces(q), w_up[part, :])
            return (silu(gate) * up).astype(jnp.bfloat16)

        def redundant_at(k, j):
            return k == 1 and j < redundant

        def run(order, far):
            first = [True]

            def begin(copy):
                if first[0]:
                    meet()
                    first[0] = False
                copy.start()

            seen = set()

            def ready(indices):
                for i in indices:
                    if i not in seen:
                        seen.add(i)
                        loads[i].wait()

            def tables():
                if "tables" not in seen:
                    seen.add("tables")
                    finish_tables()

            for step in order:
                if step == "own":
                    ready(range(6))
                    tables()
                    w_gate, w_up, w_down = wg.at[c], wu.at[c], wd.at[c]
                    own_hidden = hidden_of(lambda q: nq[q], w_gate, w_up)
                    shared_hidden = hidden_of(lambda q: nq[q], sg, su)

                    def product(cols):
                        return (
                            dot32(own_hidden, w_down[:, cols]) * weight_ref[:, 0:1]
                            + dot32(shared_hidden, sd[:, cols])
                        )

                    for j in range(2):
                        esend[j] = product(columns(2 * j + 1 - c)).astype(jnp.bfloat16)
                    begin(ecopy())
                    for j in range(2):
                        own_keep[j] = product(columns(2 * j + c))
                elif step == "pair":
                    ecopy().wait_recv()
                    own_send[...] = (
                        own_keep[1 - x] + erecv[1 - x].astype(jnp.float32)
                    ).astype(jnp.bfloat16)
                    pcopy().start()
                elif step == "wt":
                    for i in range(3):
                        ready([i])
                        begin(weight_copy(i))
                    tables()
                elif step[0] == "s":
                    j = int(step[2])
                    if step[1] == "r":
                        zred[j] = dot32(pick[0, c], nq[2 * (1 - x) + j]).astype(jnp.bfloat16)
                        begin(rcopy(j))
                    else:
                        k = 1 if step[1] == "p" else int(step[1])
                        zsend[k - 1, j] = dot32(pick[k - 1, c], nq[2 * x + j]).astype(jnp.bfloat16)
                        begin(zcopy(k, j))
                else:
                    k = 1 if step[1] == "p" else far[step[1]]
                    if step[0] == "a":
                        j = int(step[2])
                        zcopy(k, j).wait_recv()
                        if not redundant_at(k, j):
                            xcopy(k, j).start()
                    elif step[0] == "c":
                        if step == first_use(order):
                            for i in range(3):
                                weight_copy(i).wait_recv()
                        for j in range(2):
                            (rcopy(j) if redundant_at(k, j) else xcopy(k, j)).wait_recv()
                        hidden = [
                            hidden_of(lambda q: xq[k - 1, q], wg.at[d], wu.at[d]) for d in range(2)
                        ]

                        def result(cols):
                            return dot32(hidden[0], wd[0, :, cols]) + dot32(hidden[1], wd[1, :, cols])

                        for j in range(2):
                            fsend[k - 1, j] = result(columns(2 * (1 - x) + j)).astype(jnp.bfloat16)
                            fcopy(k, j).start()
                        for j in range(2):
                            keep[k - 1, j] = result(columns(2 * x + j))
                    else:
                        j = int(step[2])
                        fcopy(k, j).wait_recv()
                        gsend[k - 1, j] = (
                            keep[k - 1, j] + frecv[k - 1, j].astype(jnp.float32)
                        ).astype(jnp.bfloat16)
                        gcopy(k, j, c).start()

        inner = (e == 1) | (e == 2)

        @pl.when(inner)
        def _():
            run(INNER, {"N": 3, "F": 2})

        @pl.when(jnp.logical_not(inner))
        def _():
            run(OUTER, {"N": 2, "F": 3})

        pcopy().wait_recv()
        total = own_keep[x] + erecv[x].astype(jnp.float32) + own_recv[...].astype(jnp.float32)
        for k in LAST:
            back = 0.0
            for d in range(2):
                gcopy(k, 0, d).wait_recv()
                back = back + dot32(place[k - 1, d], grecv[k - 1, d])
            total = total + back * weight_ref[:, k:k + 1]
        out_ref[...] = total.astype(out_ref.dtype)

        for i in range(3):
            weight_copy(i).wait_send()
        ecopy().wait_send()
        pcopy().wait_send()
        for j in range(redundant):
            rcopy(j).wait_send()
        for k in (1, 2, 3):
            for j in range(2):
                zcopy(k, j).wait_send()
                if not redundant_at(k, j):
                    xcopy(k, j).wait_send()
                fcopy(k, j).wait_send()
                gcopy(k, j, c).wait_send()

    return kernel


def first_use(order):
    return [step for step in order if step[0] == "c"][0]


def fused_body(
    tokens, norm_gain, routing, gate_weights,
    expert_gate, expert_up, expert_down, shared_gate, shared_up, shared_down,
):
    rows, width = tokens.shape
    half = 3 * rows * routing.shape[1] // (2 * 4) // 2
    quarter = width // 4
    ffe = expert_gate.shape[2]
    ffs = shared_gate.shape[1]
    bf16, f32 = jnp.bfloat16, jnp.float32
    dma = pltpu.SemaphoreType.DMA
    vmem = pl.BlockSpec(memory_space=pltpu.VMEM)
    hbm = pl.BlockSpec(memory_space=pl.ANY)
    piece = (3, 2, half, quarter)
    return pl.pallas_call(
        make_kernel(half, REDUNDANT),
        out_shape=jax.ShapeDtypeStruct((rows, quarter), bf16),
        in_specs=[vmem] * 4 + [hbm] * 6,
        out_specs=vmem,
        scratch_shapes=[
            pltpu.VMEM((2, width, ffe), bf16),
            pltpu.VMEM((2, width, ffe), bf16),
            pltpu.VMEM((2, ffe, width), bf16),
            pltpu.VMEM((width, ffs), bf16),
            pltpu.VMEM((width, ffs), bf16),
            pltpu.VMEM((ffs, width), bf16),
            pltpu.VMEM((4, rows, quarter), bf16),
            pltpu.VMEM((3, 2, half, rows), bf16),
            pltpu.VMEM((3, 2, rows, half), bf16),
            pltpu.VMEM((rows, 16), f32),
            pltpu.VMEM(piece, bf16),
            pltpu.VMEM((2, half, quarter), bf16),
            pltpu.VMEM((3, 4, half, quarter), bf16),
            pltpu.VMEM((2, rows, quarter), bf16),
            pltpu.VMEM((2, rows, quarter), bf16),
            pltpu.VMEM((2, rows, quarter), f32),
            pltpu.VMEM((rows, quarter), bf16),
            pltpu.VMEM((rows, quarter), bf16),
            pltpu.VMEM(piece, bf16),
            pltpu.VMEM(piece, bf16),
            pltpu.VMEM(piece, f32),
            pltpu.VMEM(piece, bf16),
            pltpu.VMEM(piece, bf16),
            dma((6,)), dma((3,)), dma((3,)),
            dma((3, 2)), dma((3, 2)), dma((2,)), dma((2,)), dma((3, 2)), dma((3, 2)),
            dma((1,)), dma((1,)), dma((1,)), dma((1,)),
            dma((3, 2)), dma((3, 2)), dma((3, 2)), dma((3, 2)),
        ],
        compiler_params=pltpu.CompilerParams(collective_id=0, has_side_effects=True),
    )(
        tokens, norm_gain.reshape(1, width), routing.T, gate_weights.T,
        expert_gate[0], expert_up[0], expert_down[0], shared_gate, shared_up, shared_down,
    )


def solution(mesh):
    in_specs = (
        P(("grp", "ep"), None),
        P(),
        P(("grp", "ep"), None),
        P(("grp", "ep"), None),
        P("ep", None, "tp"),
        P("ep", None, "tp"),
        P("ep", "tp", None),
        P(None, "tp"),
        P(None, "tp"),
        P("tp", None),
    )
    out_specs = P(("grp", "ep"), "tp")
    ep_count, tp_count = mesh.shape["ep"], mesh.shape["tp"]

    def layer(*args):
        slots = 3 * args[0].shape[0] * args[2].shape[1] // (8 * mesh.shape["grp"] * ep_count)
        few = tp_count == 4 and ep_count == 4 and args[4].shape[0] == 4 and slots % 32 == 0
        chosen = fused_body if few else body
        return jax.shard_map(
            chosen, mesh=mesh, in_specs=in_specs, out_specs=out_specs, check_vma=False
        )(*args)

    return layer
```

```python
import jax
import jax.numpy as jnp
from jax import lax
from jax.experimental import pallas as pl
from jax.experimental.pallas import tpu as pltpu
from jax.sharding import PartitionSpec as P


def norm_rows(tokens, norm_gain):
    values = tokens.astype(jnp.float32)
    scale = lax.rsqrt(jnp.mean(values * values, axis=-1, keepdims=True) + 1e-06)
    return (values * scale * norm_gain).astype(jnp.bfloat16)


def body(
    tokens,
    norm_gain,
    routing,
    gate_weights,
    expert_gate,
    expert_up,
    expert_down,
    shared_gate,
    shared_up,
    shared_down,
):
    ep_count = lax.axis_size("ep")
    tp_count = lax.axis_size("tp")
    tok_rows, width = tokens.shape
    top = routing.shape[1]
    local_experts = expert_gate.shape[0]
    experts = ep_count * local_experts
    capacity = max(2, 3 * tok_rows * top // (2 * experts))
    quarter = width // tp_count
    arrived_rows = ep_count * capacity
    normed = norm_rows(tokens, norm_gain)
    flat_experts = routing.reshape(-1)
    assign = flat_experts.shape[0]
    onehot = (flat_experts[:, None] == jnp.arange(experts, dtype=jnp.int32)[None, :]).astype(
        jnp.float32
    )
    lower = (jnp.arange(assign)[:, None] >= jnp.arange(assign)[None, :]).astype(jnp.float32)
    running = jnp.dot(lower, onehot, precision=lax.Precision.HIGHEST)
    slot = (jnp.sum(running * onehot, axis=1) - 1.0).astype(jnp.int32)
    dest = flat_experts * capacity + slot
    owner = jnp.arange(assign, dtype=jnp.int32) // top
    slot_token = jnp.full((experts * capacity,), tok_rows, jnp.int32).at[dest].set(owner)
    padded = jnp.concatenate([normed, jnp.zeros((1, width), jnp.bfloat16)], axis=0)
    outgoing = padded[slot_token].reshape(experts, capacity, width)
    position = lax.axis_index("tp")
    own_columns = lax.dynamic_slice_in_dim(outgoing, position * quarter, quarter, 2)
    arrived = lax.all_to_all(own_columns, "ep", split_axis=0, concat_axis=0, tiled=True)
    piece = lax.all_gather(arrived, "tp", axis=2, tiled=True)
    count = piece.shape[2]
    piece = piece.reshape(ep_count, local_experts, capacity, count)
    local = 0
    rows = piece[:, local].reshape(arrived_rows, count)
    gate_rows = expert_gate[local]
    up_rows = expert_up[local]
    gate_list = [jnp.dot(rows, gate_rows, preferred_element_type=jnp.float32)]
    up_list = [jnp.dot(rows, up_rows, preferred_element_type=jnp.float32)]
    gate_all = jnp.stack(gate_list)
    up_all = jnp.stack(up_list)
    local = 0
    hidden = (jax.nn.silu(gate_all[local]) * up_all[local]).astype(jnp.bfloat16)
    term = jnp.dot(hidden, expert_down[local], preferred_element_type=jnp.float32)
    routed_list = [term.reshape(ep_count, capacity, width)]
    routed_terms = jnp.stack(routed_list, axis=1).reshape(experts * capacity, width)
    shared_gate_rows = jnp.dot(normed, shared_gate, preferred_element_type=jnp.float32)
    shared_up_rows = jnp.dot(normed, shared_up, preferred_element_type=jnp.float32)
    shared_hidden = (jax.nn.silu(shared_gate_rows) * shared_up_rows).astype(jnp.bfloat16)
    shared_term = jnp.dot(shared_hidden, shared_down, preferred_element_type=jnp.float32)
    routed_sum, shared_sum = (
        lax.psum_scatter(
            routed_terms.astype(jnp.bfloat16), "tp", scatter_dimension=1, tiled=True
        ).astype(jnp.float32),
        lax.psum_scatter(
            shared_term.astype(jnp.bfloat16), "tp", scatter_dimension=1, tiled=True
        ).astype(jnp.float32),
    )
    expert_out = routed_sum.astype(jnp.bfloat16).reshape(experts, capacity, quarter)
    returned = lax.all_to_all(expert_out, "ep", split_axis=0, concat_axis=0, tiled=True)
    picked = returned.reshape(experts * capacity, quarter)[dest]
    picked = picked.astype(jnp.float32).reshape(tok_rows, top, quarter)
    routed = jnp.sum(picked * gate_weights[:, :, None], axis=1)
    return (routed + shared_sum).astype(jnp.bfloat16)


MESH = pl.DeviceIdType.MESH


def silu(v):
    return v / (1.0 + jnp.exp(-v))


def dot32(a, b):
    return jnp.dot(a, b, preferred_element_type=jnp.float32)


OUTER = (
    "sp1", "own", "ap1", "pair", "s20", "s21", "s31", "wt", "ap0", "s30",
    "cp", "aF1", "sr0", "aF0", "gp0", "sp0", "aN0", "aN1", "cF", "gp1",
    "cN", "gF0", "gF1", "gN0", "gN1",
)
INNER = (
    "sp1", "s31", "s30", "own", "sp0", "aN1", "aN0", "ap1", "sr0", "wt",
    "aF0", "aF1", "cN", "s20", "s21", "cF", "pair", "gN0", "gN1", "ap0",
    "gF0", "gF1", "cp", "gp0", "gp1",
)
REDUNDANT = 1
LAST = (2, 3, 1)


def make_kernel(half, redundant):
    def kernel(
        tok_ref, gain_ref, routing_ref, gw_ref, wg_hbm, wu_hbm, wd_hbm, sg_hbm, su_hbm, sd_hbm,
        out_ref,
        wg, wu, wd, sg, su, sd, nq, pick, place, weight_ref,
        zsend, zred, xq, esend, erecv, own_keep, own_send, own_recv,
        fsend, frecv, keep, gsend, grecv,
        wsem, ws, wr, zs, zr, rs, rr, xs, xr, es, er, ps, pr, fs, fr, gs, gr,
    ):
        e = lax.axis_index("ep")
        t = lax.axis_index("tp")
        x = t // 2
        c = t % 2
        core = {"tp": t ^ 1}
        across = {"tp": t ^ 2}
        rows, width = tok_ref.shape
        quarter = width // 4

        barrier = pltpu.get_barrier_semaphore()
        for k in (1, 2, 3):
            for d in range(2):
                pl.semaphore_signal(
                    barrier, inc=1, device_id={"ep": e ^ k, "tp": 2 * x + d}, device_id_type=MESH
                )
        pl.semaphore_signal(barrier, inc=1, device_id=core, device_id_type=MESH)
        pl.semaphore_signal(barrier, inc=1, device_id=across, device_id_type=MESH)

        def meet():
            pl.semaphore_wait(barrier, 8)

        loads = [
            pltpu.make_async_copy(a, b, wsem.at[i])
            for i, (a, b) in enumerate(
                [
                    (wg_hbm, wg.at[c]), (wu_hbm, wu.at[c]), (wd_hbm, wd.at[c]),
                    (sg_hbm, sg), (su_hbm, su), (sd_hbm, sd),
                ]
            )
        ]
        for load in loads:
            load.start()

        values = tok_ref[...].astype(jnp.float32)
        scale = lax.rsqrt(jnp.mean(values * values, axis=-1, keepdims=True) + 1e-06)
        normed = (values * scale * gain_ref[...]).astype(jnp.bfloat16)
        for q in range(4):
            nq[q] = normed[:, q * quarter:(q + 1) * quarter]

        named = lax.broadcasted_iota(jnp.int32, (16, rows), 0) ^ e
        hit = jnp.zeros((16, rows), jnp.float32)
        weight = jnp.zeros((16, rows), jnp.float32)
        for j in range(routing_ref.shape[0]):
            same = routing_ref[j:j + 1, :] == named
            hit = hit + jnp.where(same, 1.0, 0.0)
            weight = weight + jnp.where(same, gw_ref[j:j + 1, :], 0.0)
        earlier = (
            lax.broadcasted_iota(jnp.int32, (rows, rows), 0)
            < lax.broadcasted_iota(jnp.int32, (rows, rows), 1)
        )
        earlier = jnp.where(earlier, 1.0, 0.0).astype(jnp.bfloat16)
        rank = dot32(hit.astype(jnp.bfloat16), earlier)
        rank = jnp.where(hit > 0.5, rank, -1.0)
        down = lax.broadcasted_iota(jnp.int32, (half, rows), 0).astype(jnp.float32)
        for k in (1, 2, 3):
            for d in range(2):
                pick[k - 1, d] = jnp.where(
                    rank[k:k + 1, :] == down + float(d * half), 1.0, 0.0
                ).astype(jnp.bfloat16)
        side = lax.broadcasted_iota(jnp.int32, (rows, half), 1).astype(jnp.float32)

        def finish_tables():
            weight_ref[...] = weight.T
            turned = rank.T
            for k in (1, 2, 3):
                for d in range(2):
                    place[k - 1, d] = jnp.where(
                        turned[:, k:k + 1] == side + float(d * half), 1.0, 0.0
                    ).astype(jnp.bfloat16)

        def remote(src, dst, send, recv, to):
            return pltpu.make_async_remote_copy(
                src_ref=src, dst_ref=dst, send_sem=send, recv_sem=recv,
                device_id=to, device_id_type=MESH,
            )

        def weight_copy(i):
            ref = (wg, wu, wd)[i].at[c]
            return remote(ref, ref, ws.at[i], wr.at[i], core)

        def zcopy(k, j):
            return remote(
                zsend.at[k - 1, j], xq.at[k - 1, 2 * x + j],
                zs.at[k - 1, j], zr.at[k - 1, j], {"ep": e ^ k},
            )

        def rcopy(j):
            return remote(
                zred.at[j], xq.at[0, 2 * (1 - x) + j], rs.at[j], rr.at[j], {"ep": e ^ 1}
            )

        def xcopy(k, j):
            mine = xq.at[k - 1, 2 * x + j]
            return remote(mine, mine, xs.at[k - 1, j], xr.at[k - 1, j], across)

        def ecopy():
            return remote(esend, erecv, es.at[0], er.at[0], core)

        def pcopy():
            return remote(own_send, own_recv, ps.at[0], pr.at[0], across)

        def fcopy(k, j):
            return remote(
                fsend.at[k - 1, j], frecv.at[k - 1, j],
                fs.at[k - 1, j], fr.at[k - 1, j], across,
            )

        def gcopy(k, j, d):
            return remote(
                gsend.at[k - 1, j], grecv.at[k - 1, d],
                gs.at[k - 1, j], gr.at[k - 1, d], {"ep": e ^ k, "tp": 2 * x + j},
            )

        def columns(q):
            return pl.ds(pl.multiple_of(q * quarter, quarter), quarter)

        def hidden_of(pieces, w_gate, w_up):
            gate, up = 0.0, 0.0
            for q in range(4):
                part = slice(q * quarter, (q + 1) * quarter)
                gate = gate + dot32(pieces(q), w_gate[part, :])
                up = up + dot32(pieces(q), w_up[part, :])
            return (silu(gate) * up).astype(jnp.bfloat16)

        def redundant_at(k, j):
            return k == 1 and j < redundant

        def run(order, far):
            first = [True]

            def begin(copy):
                if first[0]:
                    meet()
                    first[0] = False
                copy.start()

            seen = set()

            def ready(indices):
                for i in indices:
                    if i not in seen:
                        seen.add(i)
                        loads[i].wait()

            def tables():
                if "tables" not in seen:
                    seen.add("tables")
                    finish_tables()

            for step in order:
                if step == "own":
                    ready(range(6))
                    tables()
                    w_gate, w_up, w_down = wg.at[c], wu.at[c], wd.at[c]
                    own_hidden = hidden_of(lambda q: nq[q], w_gate, w_up)
                    shared_hidden = hidden_of(lambda q: nq[q], sg, su)

                    def product(cols):
                        return (
                            dot32(own_hidden, w_down[:, cols]) * weight_ref[:, 0:1]
                            + dot32(shared_hidden, sd[:, cols])
                        )

                    for j in range(2):
                        esend[j] = product(columns(2 * j + 1 - c)).astype(jnp.bfloat16)
                    begin(ecopy())
                    for j in range(2):
                        own_keep[j] = product(columns(2 * j + c))
                elif step == "pair":
                    ecopy().wait_recv()
                    own_send[...] = (
                        own_keep[1 - x] + erecv[1 - x].astype(jnp.float32)
                    ).astype(jnp.bfloat16)
                    pcopy().start()
                elif step == "wt":
                    for i in range(3):
                        ready([i])
                        begin(weight_copy(i))
                    tables()
                elif step[0] == "s":
                    j = int(step[2])
                    if step[1] == "r":
                        zred[j] = dot32(pick[0, c], nq[2 * (1 - x) + j]).astype(jnp.bfloat16)
                        begin(rcopy(j))
                    else:
                        k = 1 if step[1] == "p" else int(step[1])
                        zsend[k - 1, j] = dot32(pick[k - 1, c], nq[2 * x + j]).astype(jnp.bfloat16)
                        begin(zcopy(k, j))
                else:
                    k = 1 if step[1] == "p" else far[step[1]]
                    if step[0] == "a":
                        j = int(step[2])
                        zcopy(k, j).wait_recv()
                        if not redundant_at(k, j):
                            xcopy(k, j).start()
                    elif step[0] == "c":
                        if step == first_use(order):
                            for i in range(3):
                                weight_copy(i).wait_recv()
                        for j in range(2):
                            (rcopy(j) if redundant_at(k, j) else xcopy(k, j)).wait_recv()
                        hidden = [
                            hidden_of(lambda q: xq[k - 1, q], wg.at[d], wu.at[d]) for d in range(2)
                        ]

                        def result(cols):
                            return dot32(hidden[0], wd[0, :, cols]) + dot32(hidden[1], wd[1, :, cols])

                        for j in range(2):
                            fsend[k - 1, j] = result(columns(2 * (1 - x) + j)).astype(jnp.bfloat16)
                            fcopy(k, j).start()
                        for j in range(2):
                            keep[k - 1, j] = result(columns(2 * x + j))
                    else:
                        j = int(step[2])
                        fcopy(k, j).wait_recv()
                        gsend[k - 1, j] = (
                            keep[k - 1, j] + frecv[k - 1, j].astype(jnp.float32)
                        ).astype(jnp.bfloat16)
                        gcopy(k, j, c).start()

        inner = (e == 1) | (e == 2)

        @pl.when(inner)
        def _():
            run(INNER, {"N": 3, "F": 2})

        @pl.when(jnp.logical_not(inner))
        def _():
            run(OUTER, {"N": 2, "F": 3})

        pcopy().wait_recv()
        total = own_keep[x] + erecv[x].astype(jnp.float32) + own_recv[...].astype(jnp.float32)
        for k in LAST:
            back = 0.0
            for d in range(2):
                gcopy(k, 0, d).wait_recv()
                back = back + dot32(place[k - 1, d], grecv[k - 1, d])
            total = total + back * weight_ref[:, k:k + 1]
        out_ref[...] = total.astype(out_ref.dtype)

        for i in range(3):
            weight_copy(i).wait_send()
        ecopy().wait_send()
        pcopy().wait_send()
        for j in range(redundant):
            rcopy(j).wait_send()
        for k in (1, 2, 3):
            for j in range(2):
                zcopy(k, j).wait_send()
                if not redundant_at(k, j):
                    xcopy(k, j).wait_send()
                fcopy(k, j).wait_send()
                gcopy(k, j, c).wait_send()

    return kernel


def first_use(order):
    return [step for step in order if step[0] == "c"][0]


def fused_body(
    tokens, norm_gain, routing, gate_weights,
    expert_gate, expert_up, expert_down, shared_gate, shared_up, shared_down,
):
    rows, width = tokens.shape
    half = 3 * rows * routing.shape[1] // (2 * 4) // 2
    quarter = width // 4
    ffe = expert_gate.shape[2]
    ffs = shared_gate.shape[1]
    bf16, f32 = jnp.bfloat16, jnp.float32
    dma = pltpu.SemaphoreType.DMA
    vmem = pl.BlockSpec(memory_space=pltpu.VMEM)
    hbm = pl.BlockSpec(memory_space=pl.ANY)
    piece = (3, 2, half, quarter)
    return pl.pallas_call(
        make_kernel(half, REDUNDANT),
        out_shape=pltpu.VMEM((rows, quarter), bf16),
        in_specs=[vmem] * 4 + [hbm] * 6,
        out_specs=vmem,
        scratch_shapes=[
            pltpu.VMEM((2, width, ffe), bf16),
            pltpu.VMEM((2, width, ffe), bf16),
            pltpu.VMEM((2, ffe, width), bf16),
            pltpu.VMEM((width, ffs), bf16),
            pltpu.VMEM((width, ffs), bf16),
            pltpu.VMEM((ffs, width), bf16),
            pltpu.VMEM((4, rows, quarter), bf16),
            pltpu.VMEM((3, 2, half, rows), bf16),
            pltpu.VMEM((3, 2, rows, half), bf16),
            pltpu.VMEM((rows, 16), f32),
            pltpu.VMEM(piece, bf16),
            pltpu.VMEM((2, half, quarter), bf16),
            pltpu.VMEM((3, 4, half, quarter), bf16),
            pltpu.VMEM((2, rows, quarter), bf16),
            pltpu.VMEM((2, rows, quarter), bf16),
            pltpu.VMEM((2, rows, quarter), f32),
            pltpu.VMEM((rows, quarter), bf16),
            pltpu.VMEM((rows, quarter), bf16),
            pltpu.VMEM(piece, bf16),
            pltpu.VMEM(piece, bf16),
            pltpu.VMEM(piece, f32),
            pltpu.VMEM(piece, bf16),
            pltpu.VMEM(piece, bf16),
            dma((6,)), dma((3,)), dma((3,)),
            dma((3, 2)), dma((3, 2)), dma((2,)), dma((2,)), dma((3, 2)), dma((3, 2)),
            dma((1,)), dma((1,)), dma((1,)), dma((1,)),
            dma((3, 2)), dma((3, 2)), dma((3, 2)), dma((3, 2)),
        ],
        compiler_params=pltpu.CompilerParams(collective_id=0, has_side_effects=True),
    )(
        tokens, norm_gain.reshape(1, width), routing.T, gate_weights.T,
        expert_gate[0], expert_up[0], expert_down[0], shared_gate, shared_up, shared_down,
    )


def solution(mesh):
    in_specs = (
        P(("grp", "ep"), None),
        P(),
        P(("grp", "ep"), None),
        P(("grp", "ep"), None),
        P("ep", None, "tp"),
        P("ep", None, "tp"),
        P("ep", "tp", None),
        P(None, "tp"),
        P(None, "tp"),
        P("tp", None),
    )
    out_specs = P(("grp", "ep"), "tp")
    ep_count, tp_count = mesh.shape["ep"], mesh.shape["tp"]

    def layer(*args):
        slots = 3 * args[0].shape[0] * args[2].shape[1] // (8 * mesh.shape["grp"] * ep_count)
        few = tp_count == 4 and ep_count == 4 and args[4].shape[0] == 4 and slots % 32 == 0
        chosen = fused_body if few else body
        return jax.shard_map(
            chosen, mesh=mesh, in_specs=in_specs, out_specs=out_specs, check_vma=False
        )(*args)

    return layer
```

```python
import jax
import jax.numpy as jnp
from jax import lax
from jax.experimental import pallas as pl
from jax.experimental.pallas import tpu as pltpu
from jax.sharding import PartitionSpec as P


def norm_rows(tokens, norm_gain):
    values = tokens.astype(jnp.float32)
    scale = lax.rsqrt(jnp.mean(values * values, axis=-1, keepdims=True) + 1e-06)
    return (values * scale * norm_gain).astype(jnp.bfloat16)


def body(
    tokens,
    norm_gain,
    routing,
    gate_weights,
    expert_gate,
    expert_up,
    expert_down,
    shared_gate,
    shared_up,
    shared_down,
):
    ep_count = lax.axis_size("ep")
    tp_count = lax.axis_size("tp")
    tok_rows, width = tokens.shape
    top = routing.shape[1]
    local_experts = expert_gate.shape[0]
    experts = ep_count * local_experts
    capacity = max(2, 3 * tok_rows * top // (2 * experts))
    quarter = width // tp_count
    arrived_rows = ep_count * capacity
    normed = norm_rows(tokens, norm_gain)
    flat_experts = routing.reshape(-1)
    assign = flat_experts.shape[0]
    onehot = (flat_experts[:, None] == jnp.arange(experts, dtype=jnp.int32)[None, :]).astype(
        jnp.float32
    )
    lower = (jnp.arange(assign)[:, None] >= jnp.arange(assign)[None, :]).astype(jnp.float32)
    running = jnp.dot(lower, onehot, precision=lax.Precision.HIGHEST)
    slot = (jnp.sum(running * onehot, axis=1) - 1.0).astype(jnp.int32)
    dest = flat_experts * capacity + slot
    owner = jnp.arange(assign, dtype=jnp.int32) // top
    slot_token = jnp.full((experts * capacity,), tok_rows, jnp.int32).at[dest].set(owner)
    padded = jnp.concatenate([normed, jnp.zeros((1, width), jnp.bfloat16)], axis=0)
    outgoing = padded[slot_token].reshape(experts, capacity, width)
    position = lax.axis_index("tp")
    own_columns = lax.dynamic_slice_in_dim(outgoing, position * quarter, quarter, 2)
    arrived = lax.all_to_all(own_columns, "ep", split_axis=0, concat_axis=0, tiled=True)
    piece = lax.all_gather(arrived, "tp", axis=2, tiled=True)
    count = piece.shape[2]
    piece = piece.reshape(ep_count, local_experts, capacity, count)
    local = 0
    rows = piece[:, local].reshape(arrived_rows, count)
    gate_rows = expert_gate[local]
    up_rows = expert_up[local]
    gate_list = [jnp.dot(rows, gate_rows, preferred_element_type=jnp.float32)]
    up_list = [jnp.dot(rows, up_rows, preferred_element_type=jnp.float32)]
    gate_all = jnp.stack(gate_list)
    up_all = jnp.stack(up_list)
    local = 0
    hidden = (jax.nn.silu(gate_all[local]) * up_all[local]).astype(jnp.bfloat16)
    term = jnp.dot(hidden, expert_down[local], preferred_element_type=jnp.float32)
    routed_list = [term.reshape(ep_count, capacity, width)]
    routed_terms = jnp.stack(routed_list, axis=1).reshape(experts * capacity, width)
    shared_gate_rows = jnp.dot(normed, shared_gate, preferred_element_type=jnp.float32)
    shared_up_rows = jnp.dot(normed, shared_up, preferred_element_type=jnp.float32)
    shared_hidden = (jax.nn.silu(shared_gate_rows) * shared_up_rows).astype(jnp.bfloat16)
    shared_term = jnp.dot(shared_hidden, shared_down, preferred_element_type=jnp.float32)
    routed_sum, shared_sum = (
        lax.psum_scatter(
            routed_terms.astype(jnp.bfloat16), "tp", scatter_dimension=1, tiled=True
        ).astype(jnp.float32),
        lax.psum_scatter(
            shared_term.astype(jnp.bfloat16), "tp", scatter_dimension=1, tiled=True
        ).astype(jnp.float32),
    )
    expert_out = routed_sum.astype(jnp.bfloat16).reshape(experts, capacity, quarter)
    returned = lax.all_to_all(expert_out, "ep", split_axis=0, concat_axis=0, tiled=True)
    picked = returned.reshape(experts * capacity, quarter)[dest]
    picked = picked.astype(jnp.float32).reshape(tok_rows, top, quarter)
    routed = jnp.sum(picked * gate_weights[:, :, None], axis=1)
    return (routed + shared_sum).astype(jnp.bfloat16)


MESH = pl.DeviceIdType.MESH


def silu(v):
    return v / (1.0 + jnp.exp(-v))


def dot32(a, b):
    return jnp.dot(a, b, preferred_element_type=jnp.float32)


OUTER = (
    "s20", "sp3", "s30", "s32", "s22", "ap3", "s23", "s21", "wt", "sp2",
    "ap2", "ap1", "sp0", "aF2", "s33", "s31", "sp1", "aF0", "ap0", "cp",
    "sr0", "gp0", "gp1", "aF3", "sr1", "aF1", "own", "aN3", "aN2", "aN0",
    "aN1", "cF", "cN", "pair", "gp3", "gp2", "gF1", "gF0", "gF3", "gN0",
    "gF2", "gN2", "gN3", "gN1",
)
INNER = (
    "s33", "sp3", "wt", "far", "sr0", "sp2", "s30", "aN3", "sp1", "s32",
    "ap3", "aF0", "s23", "s31", "sp0", "sr1", "aF1", "aN0", "s22", "aF2",
    "aF3", "aN2", "ap2", "s20", "aN1", "cF", "ap1", "s21", "own", "cN",
    "gF0", "gF2", "gF3", "gF1", "gN0", "ap0", "gN2", "cp", "gN3", "gN1",
    "gp0", "pair", "gp3", "gp1", "gp2",
)
CHUNKS = 4
REDUNDANT = 2
LAST = (2, 3, 1)


def make_kernel(half, redundant, chunks):
    def kernel(
        tok_ref, gain_ref, routing_ref, gw_ref, wg_hbm, wu_hbm, wd_hbm, sg_hbm, su_hbm, sd_hbm,
        out_ref,
        wg, wu, wd, sg, su, sd, nq, pick, place, weight_ref,
        zsend, zred, xq, esend, erecv, own_keep, own_send, own_recv,
        fsend, frecv, keep, gsend, grecv,
        wsem, far_sem, ws, wr, zs, zr, rs, rr, xs, xr, es, er, ps, pr, fs, fr, gs, gr,
    ):
        e = lax.axis_index("ep")
        t = lax.axis_index("tp")
        x = t // 2
        c = t % 2
        core = {"tp": t ^ 1}
        across = {"tp": t ^ 2}
        rows, width = tok_ref.shape
        quarter = width // 4
        part = chunks // 2
        wide = quarter // part
        inner = (e == 1) | (e == 2)

        barrier = pltpu.get_barrier_semaphore()

        def greet(k):
            for d in range(2):
                pl.semaphore_signal(
                    barrier, inc=1, device_id={"ep": e ^ k, "tp": 2 * x + d}, device_id_type=MESH
                )

        greet(1)
        pl.semaphore_signal(barrier, inc=1, device_id=core, device_id_type=MESH)
        pl.semaphore_signal(barrier, inc=1, device_id=across, device_id_type=MESH)

        @pl.when(inner)
        def _():
            greet(3)

        def tell(i, k):
            pl.semaphore_signal(
                far_sem.at[i], inc=1, device_id={"ep": e ^ k}, device_id_type=MESH
            )

        loads = [
            pltpu.make_async_copy(a, b, wsem.at[i])
            for i, (a, b) in enumerate(
                [
                    (wg_hbm, wg.at[c]), (wu_hbm, wu.at[c]), (wd_hbm, wd.at[c]),
                    (sg_hbm, sg), (su_hbm, su), (sd_hbm, sd),
                ]
            )
        ]
        for load in loads:
            load.start()

        values = tok_ref[...].astype(jnp.float32)
        scale = lax.rsqrt(jnp.mean(values * values, axis=-1, keepdims=True) + 1e-06)
        nq[...] = (values * scale * gain_ref[...]).astype(jnp.bfloat16)

        named = lax.broadcasted_iota(jnp.int32, (16, rows), 0) ^ e
        hit = jnp.zeros((16, rows), jnp.float32)
        weight = jnp.zeros((16, rows), jnp.float32)
        for j in range(routing_ref.shape[0]):
            same = routing_ref[j:j + 1, :] == named
            hit = hit + jnp.where(same, 1.0, 0.0)
            weight = weight + jnp.where(same, gw_ref[j:j + 1, :], 0.0)
        earlier = (
            lax.broadcasted_iota(jnp.int32, (rows, rows), 0)
            < lax.broadcasted_iota(jnp.int32, (rows, rows), 1)
        )
        earlier = jnp.where(earlier, 1.0, 0.0).astype(jnp.bfloat16)
        rank = dot32(hit.astype(jnp.bfloat16), earlier)
        rank = jnp.where(hit > 0.5, rank, -1.0)
        down = lax.broadcasted_iota(jnp.int32, (half, rows), 0).astype(jnp.float32)
        for k in (1, 2, 3):
            for d in range(2):
                pick[k - 1, d] = jnp.where(
                    rank[k:k + 1, :] == down + float(d * half), 1.0, 0.0
                ).astype(jnp.bfloat16)
        side = lax.broadcasted_iota(jnp.int32, (rows, half), 1).astype(jnp.float32)

        def finish_tables():
            weight_ref[...] = weight.T
            turned = rank.T
            for k in (1, 2, 3):
                for d in range(2):
                    place[k - 1, d] = jnp.where(
                        turned[:, k:k + 1] == side + float(d * half), 1.0, 0.0
                    ).astype(jnp.bfloat16)

        def remote(src, dst, send, recv, to):
            return pltpu.make_async_remote_copy(
                src_ref=src, dst_ref=dst, send_sem=send, recv_sem=recv,
                device_id=to, device_id_type=MESH,
            )

        def weight_copy(i):
            ref = (wg, wu, wd)[i].at[c]
            return remote(ref, ref, ws.at[i], wr.at[i], core)

        def zcopy(k, j):
            return remote(
                zsend.at[k - 1, j], xq.at[k - 1, chunks * x + j],
                zs.at[k - 1, j], zr.at[k - 1, j], {"ep": e ^ k},
            )

        def rcopy(j):
            return remote(
                zred.at[j], xq.at[0, chunks * (1 - x) + j], rs.at[j], rr.at[j], {"ep": e ^ 1}
            )

        def xcopy(k, j):
            mine = xq.at[k - 1, chunks * x + j]
            return remote(mine, mine, xs.at[k - 1, j], xr.at[k - 1, j], across)

        def ecopy():
            return remote(esend, erecv, es.at[0], er.at[0], core)

        def pcopy():
            return remote(own_send, own_recv, ps.at[0], pr.at[0], across)

        def fcopy(k, j):
            return remote(
                fsend.at[k - 1, j], frecv.at[k - 1, j],
                fs.at[k - 1, j], fr.at[k - 1, j], across,
            )

        def gcopy(k, j, d):
            return remote(
                gsend.at[k - 1, j], grecv.at[k - 1, d, j % part],
                gs.at[k - 1, j], gr.at[k - 1, d, j % part],
                {"ep": e ^ k, "tp": 2 * x + j // part},
            )

        def columns(q, size):
            return pl.ds(pl.multiple_of(q * size, size), size)

        def hidden_of(values, w_gate, w_up):
            gate = dot32(values, w_gate[...])
            up = dot32(values, w_up[...])
            return (silu(gate) * up).astype(jnp.bfloat16)

        def redundant_at(k, j):
            return k == 1 and j < redundant

        def run(order, far, middle):
            seen = set()

            def begin(copy):
                if "meet" not in seen:
                    seen.add("meet")
                    pl.semaphore_wait(barrier, 6 if middle else 4)
                    if middle:
                        tell(0, 1)
                        tell(0, 3)
                copy.start()

            def know(k):
                if ("far", k) not in seen and (k == 2 or (k == 3 and not middle)):
                    seen.add(("far", k))
                    pl.semaphore_wait(far_sem.at[k - 2], 1)
                    if middle:
                        tell(1, 1)

            def ready(indices):
                for i in indices:
                    if i not in seen:
                        seen.add(i)
                        loads[i].wait()

            def tables():
                if "tables" not in seen:
                    seen.add("tables")
                    finish_tables()

            for step in order:
                if step == "far":
                    know(2)
                elif step == "own":
                    ready(range(6))
                    tables()
                    w_gate, w_up, w_down = wg.at[c], wu.at[c], wd.at[c]
                    own_hidden = hidden_of(nq[...], w_gate, w_up)
                    shared_hidden = hidden_of(nq[...], sg, su)

                    def product(cols):
                        return (
                            dot32(own_hidden, w_down[:, cols]) * weight_ref[:, 0:1]
                            + dot32(shared_hidden, sd[:, cols])
                        )

                    for j in range(2):
                        esend[j] = product(columns(2 * j + 1 - c, quarter)).astype(jnp.bfloat16)
                    begin(ecopy())
                    for j in range(2):
                        own_keep[j] = product(columns(2 * j + c, quarter))
                elif step == "pair":
                    ecopy().wait_recv()
                    own_send[...] = (
                        own_keep[1 - x] + erecv[1 - x].astype(jnp.float32)
                    ).astype(jnp.bfloat16)
                    pcopy().start()
                elif step == "wt":
                    for i in range(3):
                        ready([i])
                        begin(weight_copy(i))
                    tables()
                elif step[0] == "s":
                    j = int(step[2])
                    if step[1] == "r":
                        zred[j] = dot32(
                            pick[0, c], nq[:, columns(chunks * (1 - x) + j, wide)]
                        ).astype(jnp.bfloat16)
                        begin(rcopy(j))
                    else:
                        k = 1 if step[1] == "p" else int(step[1])
                        zsend[k - 1, j] = dot32(
                            pick[k - 1, c], nq[:, columns(chunks * x + j, wide)]
                        ).astype(jnp.bfloat16)
                        if "meet" in seen:
                            know(k)
                            begin(zcopy(k, j))
                        else:
                            copy = zcopy(k, j)
                            begin(NoCopy())
                            know(k)
                            copy.start()
                else:
                    k = 1 if step[1] == "p" else far[step[1]]
                    if step[0] == "a":
                        j = int(step[2])
                        zcopy(k, j).wait_recv()
                        if not redundant_at(k, j):
                            xcopy(k, j).start()
                    elif step[0] == "c":
                        if step == first_use(order):
                            for i in range(3):
                                weight_copy(i).wait_recv()
                        for j in range(chunks):
                            (rcopy(j) if redundant_at(k, j) else xcopy(k, j)).wait_recv()
                        rows_in = jnp.concatenate([xq[k - 1, q] for q in range(2 * chunks)], axis=1)
                        hidden = [hidden_of(rows_in, wg.at[d], wu.at[d]) for d in range(2)]

                        def result(cols):
                            return dot32(hidden[0], wd[0, :, cols]) + dot32(hidden[1], wd[1, :, cols])

                        for j in range(chunks):
                            fsend[k - 1, j] = result(
                                columns(chunks * (1 - x) + j, wide)
                            ).astype(jnp.bfloat16)
                            fcopy(k, j).start()
                        for j in range(chunks):
                            keep[k - 1, j] = result(columns(chunks * x + j, wide))
                    else:
                        j = int(step[2])
                        fcopy(k, j).wait_recv()
                        gsend[k - 1, j] = (
                            keep[k - 1, j] + frecv[k - 1, j].astype(jnp.float32)
                        ).astype(jnp.bfloat16)
                        gcopy(k, j, c).start()

        @pl.when(inner)
        def _():
            run(INNER, {"N": 3, "F": 2}, True)

        @pl.when(jnp.logical_not(inner))
        def _():
            run(OUTER, {"N": 2, "F": 3}, False)

        pcopy().wait_recv()
        total = own_keep[x] + erecv[x].astype(jnp.float32) + own_recv[...].astype(jnp.float32)
        for k in LAST:
            back = 0.0
            for d in range(2):
                for j in range(part):
                    gcopy(k, j, d).wait_recv()
                returned = jnp.concatenate([grecv[k - 1, d, j] for j in range(part)], axis=1)
                back = back + dot32(place[k - 1, d], returned)
            total = total + back * weight_ref[:, k:k + 1]
        out_ref[...] = total.astype(out_ref.dtype)

        for i in range(3):
            weight_copy(i).wait_send()
        ecopy().wait_send()
        pcopy().wait_send()
        for j in range(redundant):
            rcopy(j).wait_send()
        for k in (1, 2, 3):
            for j in range(chunks):
                zcopy(k, j).wait_send()
                if not redundant_at(k, j):
                    xcopy(k, j).wait_send()
                fcopy(k, j).wait_send()
                gcopy(k, j, c).wait_send()

    return kernel


class NoCopy:
    def start(self):
        pass


def first_use(order):
    return [step for step in order if step[0] == "c"][0]


def fused_body(
    tokens, norm_gain, routing, gate_weights,
    expert_gate, expert_up, expert_down, shared_gate, shared_up, shared_down,
):
    rows, width = tokens.shape
    half = 3 * rows * routing.shape[1] // (2 * 4) // 2
    quarter = width // 4
    ffe = expert_gate.shape[2]
    ffs = shared_gate.shape[1]
    bf16, f32 = jnp.bfloat16, jnp.float32
    dma = pltpu.SemaphoreType.DMA
    vmem = pl.BlockSpec(memory_space=pltpu.VMEM)
    hbm = pl.BlockSpec(memory_space=pl.ANY)
    chunks = CHUNKS
    wide = 2 * quarter // chunks
    piece = (3, chunks, half, wide)
    return pl.pallas_call(
        make_kernel(half, REDUNDANT, chunks),
        out_shape=pltpu.VMEM((rows, quarter), bf16),
        in_specs=[vmem] * 4 + [hbm] * 6,
        out_specs=vmem,
        scratch_shapes=[
            pltpu.VMEM((2, width, ffe), bf16),
            pltpu.VMEM((2, width, ffe), bf16),
            pltpu.VMEM((2, ffe, width), bf16),
            pltpu.VMEM((width, ffs), bf16),
            pltpu.VMEM((width, ffs), bf16),
            pltpu.VMEM((ffs, width), bf16),
            pltpu.VMEM((rows, width), bf16),
            pltpu.VMEM((3, 2, half, rows), bf16),
            pltpu.VMEM((3, 2, rows, half), bf16),
            pltpu.VMEM((rows, 16), f32),
            pltpu.VMEM(piece, bf16),
            pltpu.VMEM((max(REDUNDANT, 1), half, wide), bf16),
            pltpu.VMEM((3, 2 * chunks, half, wide), bf16),
            pltpu.VMEM((2, rows, quarter), bf16),
            pltpu.VMEM((2, rows, quarter), bf16),
            pltpu.VMEM((2, rows, quarter), f32),
            pltpu.VMEM((rows, quarter), bf16),
            pltpu.VMEM((rows, quarter), bf16),
            pltpu.VMEM(piece, bf16),
            pltpu.VMEM(piece, bf16),
            pltpu.VMEM(piece, f32),
            pltpu.VMEM(piece, bf16),
            pltpu.VMEM((3, 2, chunks // 2, half, wide), bf16),
            dma((6,)), pltpu.SemaphoreType.REGULAR((2,)), dma((3,)), dma((3,)),
            dma((3, chunks)), dma((3, chunks)), dma((chunks,)), dma((chunks,)),
            dma((3, chunks)), dma((3, chunks)),
            dma((1,)), dma((1,)), dma((1,)), dma((1,)),
            dma((3, chunks)), dma((3, chunks)), dma((3, chunks)), dma((3, 2, chunks // 2)),
        ],
        compiler_params=pltpu.CompilerParams(collective_id=0, has_side_effects=True),
    )(
        tokens, norm_gain.reshape(1, width), routing.T, gate_weights.T,
        expert_gate[0], expert_up[0], expert_down[0], shared_gate, shared_up, shared_down,
    )


def solution(mesh):
    in_specs = (
        P(("grp", "ep"), None),
        P(),
        P(("grp", "ep"), None),
        P(("grp", "ep"), None),
        P("ep", None, "tp"),
        P("ep", None, "tp"),
        P("ep", "tp", None),
        P(None, "tp"),
        P(None, "tp"),
        P("tp", None),
    )
    out_specs = P(("grp", "ep"), "tp")
    ep_count, tp_count = mesh.shape["ep"], mesh.shape["tp"]

    def layer(*args):
        slots = 3 * args[0].shape[0] * args[2].shape[1] // (8 * mesh.shape["grp"] * ep_count)
        few = tp_count == 4 and ep_count == 4 and args[4].shape[0] == 4 and slots % 32 == 0
        chosen = fused_body if few else body
        return jax.shard_map(
            chosen, mesh=mesh, in_specs=in_specs, out_specs=out_specs, check_vma=False
        )(*args)

    return layer
```

```python
import jax
import jax.numpy as jnp
from jax import lax
from jax.experimental import pallas as pl
from jax.experimental.pallas import tpu as pltpu
from jax.sharding import PartitionSpec as P


def norm_rows(tokens, norm_gain):
    values = tokens.astype(jnp.float32)
    scale = lax.rsqrt(jnp.mean(values * values, axis=-1, keepdims=True) + 1e-06)
    return (values * scale * norm_gain).astype(jnp.bfloat16)


def body(
    tokens,
    norm_gain,
    routing,
    gate_weights,
    expert_gate,
    expert_up,
    expert_down,
    shared_gate,
    shared_up,
    shared_down,
):
    ep_count = lax.axis_size("ep")
    tp_count = lax.axis_size("tp")
    tok_rows, width = tokens.shape
    top = routing.shape[1]
    local_experts = expert_gate.shape[0]
    experts = ep_count * local_experts
    capacity = max(2, 3 * tok_rows * top // (2 * experts))
    quarter = width // tp_count
    arrived_rows = ep_count * capacity
    normed = norm_rows(tokens, norm_gain)
    flat_experts = routing.reshape(-1)
    assign = flat_experts.shape[0]
    onehot = (flat_experts[:, None] == jnp.arange(experts, dtype=jnp.int32)[None, :]).astype(
        jnp.float32
    )
    lower = (jnp.arange(assign)[:, None] >= jnp.arange(assign)[None, :]).astype(jnp.float32)
    running = jnp.dot(lower, onehot, precision=lax.Precision.HIGHEST)
    slot = (jnp.sum(running * onehot, axis=1) - 1.0).astype(jnp.int32)
    dest = flat_experts * capacity + slot
    owner = jnp.arange(assign, dtype=jnp.int32) // top
    slot_token = jnp.full((experts * capacity,), tok_rows, jnp.int32).at[dest].set(owner)
    padded = jnp.concatenate([normed, jnp.zeros((1, width), jnp.bfloat16)], axis=0)
    outgoing = padded[slot_token].reshape(experts, capacity, width)
    position = lax.axis_index("tp")
    own_columns = lax.dynamic_slice_in_dim(outgoing, position * quarter, quarter, 2)
    arrived = lax.all_to_all(own_columns, "ep", split_axis=0, concat_axis=0, tiled=True)
    piece = lax.all_gather(arrived, "tp", axis=2, tiled=True)
    count = piece.shape[2]
    piece = piece.reshape(ep_count, local_experts, capacity, count)
    local = 0
    rows = piece[:, local].reshape(arrived_rows, count)
    gate_rows = expert_gate[local]
    up_rows = expert_up[local]
    gate_list = [jnp.dot(rows, gate_rows, preferred_element_type=jnp.float32)]
    up_list = [jnp.dot(rows, up_rows, preferred_element_type=jnp.float32)]
    gate_all = jnp.stack(gate_list)
    up_all = jnp.stack(up_list)
    local = 0
    hidden = (jax.nn.silu(gate_all[local]) * up_all[local]).astype(jnp.bfloat16)
    term = jnp.dot(hidden, expert_down[local], preferred_element_type=jnp.float32)
    routed_list = [term.reshape(ep_count, capacity, width)]
    routed_terms = jnp.stack(routed_list, axis=1).reshape(experts * capacity, width)
    shared_gate_rows = jnp.dot(normed, shared_gate, preferred_element_type=jnp.float32)
    shared_up_rows = jnp.dot(normed, shared_up, preferred_element_type=jnp.float32)
    shared_hidden = (jax.nn.silu(shared_gate_rows) * shared_up_rows).astype(jnp.bfloat16)
    shared_term = jnp.dot(shared_hidden, shared_down, preferred_element_type=jnp.float32)
    routed_sum, shared_sum = (
        lax.psum_scatter(
            routed_terms.astype(jnp.bfloat16), "tp", scatter_dimension=1, tiled=True
        ).astype(jnp.float32),
        lax.psum_scatter(
            shared_term.astype(jnp.bfloat16), "tp", scatter_dimension=1, tiled=True
        ).astype(jnp.float32),
    )
    expert_out = routed_sum.astype(jnp.bfloat16).reshape(experts, capacity, quarter)
    returned = lax.all_to_all(expert_out, "ep", split_axis=0, concat_axis=0, tiled=True)
    picked = returned.reshape(experts * capacity, quarter)[dest]
    picked = picked.astype(jnp.float32).reshape(tok_rows, top, quarter)
    routed = jnp.sum(picked * gate_weights[:, :, None], axis=1)
    return (routed + shared_sum).astype(jnp.bfloat16)


MESH = pl.DeviceIdType.MESH


def silu(v):
    return v / (1.0 + jnp.exp(-v))


def dot32(a, b):
    return jnp.dot(a, b, preferred_element_type=jnp.float32)


OUTER = (
    "own", "s21", "s20", "sp1", "pair", "sr0", "s31", "aN0", "aN1", "s30",
    "ap1", "ap0", "wt", "aF1", "sp0", "aF0", "cN", "cF", "gN0", "cp",
    "gN1", "gF0", "gF1", "gp0", "gp1",
)
INNER = (
    "sp1", "far", "wt", "s20", "own", "sp0", "s21", "aF1", "sr0", "s31",
    "aF0", "ap1", "s30", "cF", "aN1", "ap0", "gF0", "gF1", "aN0", "cp",
    "cN", "gp0", "gN0", "pair", "gp1", "gN1",
)
CHUNKS = 2
REDUNDANT = 1
LAST = (2, 3, 1)


def make_kernel(half, redundant, chunks):
    def kernel(
        tok_ref, gain_ref, routing_ref, gw_ref, wg_hbm, wu_hbm, wd_hbm, sg_hbm, su_hbm, sd_hbm,
        out_ref,
        wg, wu, wd, sg, su, sd, nq, pick, place, weight_ref,
        zsend, zred, xq, esend, erecv, own_keep, own_send, own_recv,
        fsend, frecv, keep, gsend, grecv,
        wsem, far_sem, ws, wr, zs, zr, rs, rr, xs, xr, es, er, ps, pr, fs, fr, gs, gr,
    ):
        e = lax.axis_index("ep")
        t = lax.axis_index("tp")
        x = t // 2
        c = t % 2
        core = {"tp": t ^ 1}
        across = {"tp": t ^ 2}
        rows, width = tok_ref.shape
        quarter = width // 4
        part = chunks // 2
        wide = quarter // part
        inner = (e == 1) | (e == 2)

        barrier = pltpu.get_barrier_semaphore()

        def greet(k):
            for d in range(2):
                pl.semaphore_signal(
                    barrier, inc=1, device_id={"ep": e ^ k, "tp": 2 * x + d}, device_id_type=MESH
                )

        greet(1)
        pl.semaphore_signal(barrier, inc=1, device_id=core, device_id_type=MESH)
        pl.semaphore_signal(barrier, inc=1, device_id=across, device_id_type=MESH)

        @pl.when(inner)
        def _():
            greet(3)

        def tell(i, k):
            pl.semaphore_signal(
                far_sem.at[i], inc=1, device_id={"ep": e ^ k}, device_id_type=MESH
            )

        loads = [
            pltpu.make_async_copy(a, b, wsem.at[i])
            for i, (a, b) in enumerate(
                [
                    (wg_hbm, wg.at[c]), (wu_hbm, wu.at[c]), (wd_hbm, wd.at[c]),
                    (sg_hbm, sg), (su_hbm, su), (sd_hbm, sd),
                ]
            )
        ]
        for load in loads:
            load.start()

        values = tok_ref[...].astype(jnp.float32)
        scale = lax.rsqrt(jnp.mean(values * values, axis=-1, keepdims=True) + 1e-06)
        nq[...] = (values * scale * gain_ref[...]).astype(jnp.bfloat16)

        named = lax.broadcasted_iota(jnp.int32, (16, rows), 0) ^ e
        hit = jnp.zeros((16, rows), jnp.float32)
        weight = jnp.zeros((16, rows), jnp.float32)
        for j in range(routing_ref.shape[0]):
            same = routing_ref[j:j + 1, :] == named
            hit = hit + jnp.where(same, 1.0, 0.0)
            weight = weight + jnp.where(same, gw_ref[j:j + 1, :], 0.0)
        earlier = (
            lax.broadcasted_iota(jnp.int32, (rows, rows), 0)
            < lax.broadcasted_iota(jnp.int32, (rows, rows), 1)
        )
        earlier = jnp.where(earlier, 1.0, 0.0).astype(jnp.bfloat16)
        rank = dot32(hit.astype(jnp.bfloat16), earlier)
        rank = jnp.where(hit > 0.5, rank, -1.0)
        down = lax.broadcasted_iota(jnp.int32, (half, rows), 0).astype(jnp.float32)
        for k in (1, 2, 3):
            for d in range(2):
                pick[k - 1, d] = jnp.where(
                    rank[k:k + 1, :] == down + float(d * half), 1.0, 0.0
                ).astype(jnp.bfloat16)
        side = lax.broadcasted_iota(jnp.int32, (rows, half), 1).astype(jnp.float32)

        def finish_tables():
            weight_ref[...] = weight.T
            turned = rank.T
            for k in (1, 2, 3):
                for d in range(2):
                    place[k - 1, d] = jnp.where(
                        turned[:, k:k + 1] == side + float(d * half), 1.0, 0.0
                    ).astype(jnp.bfloat16)

        def remote(src, dst, send, recv, to):
            return pltpu.make_async_remote_copy(
                src_ref=src, dst_ref=dst, send_sem=send, recv_sem=recv,
                device_id=to, device_id_type=MESH,
            )

        def weight_copy(i):
            ref = (wg, wu, wd)[i].at[c]
            return remote(ref, ref, ws.at[i], wr.at[i], core)

        def zcopy(k, j):
            return remote(
                zsend.at[k - 1, j], xq.at[k - 1, chunks * x + j],
                zs.at[k - 1, j], zr.at[k - 1, j], {"ep": e ^ k},
            )

        def rcopy(j):
            return remote(
                zred.at[j], xq.at[0, chunks * (1 - x) + j], rs.at[j], rr.at[j], {"ep": e ^ 1}
            )

        def xcopy(k, j):
            mine = xq.at[k - 1, chunks * x + j]
            return remote(mine, mine, xs.at[k - 1, j], xr.at[k - 1, j], across)

        def ecopy():
            return remote(esend, erecv, es.at[0], er.at[0], core)

        def pcopy():
            return remote(own_send, own_recv, ps.at[0], pr.at[0], across)

        def fcopy(k, j):
            return remote(
                fsend.at[k - 1, j], frecv.at[k - 1, j],
                fs.at[k - 1, j], fr.at[k - 1, j], across,
            )

        def gcopy(k, j, d):
            return remote(
                gsend.at[k - 1, j], grecv.at[k - 1, d, j % part],
                gs.at[k - 1, j], gr.at[k - 1, d, j % part],
                {"ep": e ^ k, "tp": 2 * x + j // part},
            )

        def columns(q, size):
            return pl.ds(pl.multiple_of(q * size, size), size)

        def hidden_of(values, w_gate, w_up):
            gate = dot32(values, w_gate[...])
            up = dot32(values, w_up[...])
            return (silu(gate) * up).astype(jnp.bfloat16)

        def redundant_at(k, j):
            return k == 1 and j < redundant

        def run(order, far, middle):
            seen = set()

            def begin(copy):
                if "meet" not in seen:
                    seen.add("meet")
                    pl.semaphore_wait(barrier, 6 if middle else 4)
                    if middle:
                        tell(0, 1)
                        tell(0, 3)
                copy.start()

            def know(k):
                if ("far", k) not in seen and (k == 2 or (k == 3 and not middle)):
                    seen.add(("far", k))
                    pl.semaphore_wait(far_sem.at[k - 2], 1)
                    if middle:
                        tell(1, 1)

            def ready(indices):
                for i in indices:
                    if i not in seen:
                        seen.add(i)
                        loads[i].wait()

            def tables():
                if "tables" not in seen:
                    seen.add("tables")
                    finish_tables()

            for step in order:
                if step == "far":
                    know(2)
                elif step == "own":
                    ready(range(6))
                    tables()
                    w_gate, w_up, w_down = wg.at[c], wu.at[c], wd.at[c]
                    own_hidden = hidden_of(nq[...], w_gate, w_up)
                    shared_hidden = hidden_of(nq[...], sg, su)

                    def product(cols):
                        return (
                            dot32(own_hidden, w_down[:, cols]) * weight_ref[:, 0:1]
                            + dot32(shared_hidden, sd[:, cols])
                        )

                    for j in range(2):
                        esend[j] = product(columns(2 * j + 1 - c, quarter)).astype(jnp.bfloat16)
                    begin(ecopy())
                    for j in range(2):
                        own_keep[j] = product(columns(2 * j + c, quarter))
                elif step == "pair":
                    ecopy().wait_recv()
                    own_send[...] = (
                        own_keep[1 - x] + erecv[1 - x].astype(jnp.float32)
                    ).astype(jnp.bfloat16)
                    pcopy().start()
                elif step == "wt":
                    for i in range(3):
                        ready([i])
                        begin(weight_copy(i))
                    tables()
                elif step[0] == "s":
                    j = int(step[2])
                    if step[1] == "r":
                        zred[j] = dot32(
                            pick[0, c], nq[:, columns(chunks * (1 - x) + j, wide)]
                        ).astype(jnp.bfloat16)
                        begin(rcopy(j))
                    else:
                        k = 1 if step[1] == "p" else int(step[1])
                        zsend[k - 1, j] = dot32(
                            pick[k - 1, c], nq[:, columns(chunks * x + j, wide)]
                        ).astype(jnp.bfloat16)
                        if "meet" in seen:
                            know(k)
                            begin(zcopy(k, j))
                        else:
                            copy = zcopy(k, j)
                            begin(NoCopy())
                            know(k)
                            copy.start()
                else:
                    k = 1 if step[1] == "p" else far[step[1]]
                    if step[0] == "a":
                        j = int(step[2])
                        zcopy(k, j).wait_recv()
                        if not redundant_at(k, j):
                            xcopy(k, j).start()
                    elif step[0] == "c":
                        if step == first_use(order):
                            for i in range(3):
                                weight_copy(i).wait_recv()
                        gates, ups = [0.0, 0.0], [0.0, 0.0]
                        for side_x in (x, 1 - x):
                            if side_x is not x:
                                for j in range(chunks):
                                    (rcopy(j) if redundant_at(k, j) else xcopy(k, j)).wait_recv()
                            part_in = jnp.concatenate(
                                [xq[k - 1, chunks * side_x + q] for q in range(chunks)], axis=1
                            )
                            deep = columns(side_x, width // 2)
                            for d in range(2):
                                gates[d] = gates[d] + dot32(part_in, wg[d, deep, :])
                                ups[d] = ups[d] + dot32(part_in, wu[d, deep, :])
                        hidden = jnp.concatenate(
                            [(silu(gates[d]) * ups[d]).astype(jnp.bfloat16) for d in range(2)], axis=1
                        )

                        def result(cols):
                            both = jnp.concatenate([wd[0, :, cols], wd[1, :, cols]], axis=0)
                            return dot32(hidden, both)

                        for j in range(chunks):
                            fsend[k - 1, j] = result(
                                columns(chunks * (1 - x) + j, wide)
                            ).astype(jnp.bfloat16)
                            fcopy(k, j).start()
                        for j in range(chunks):
                            keep[k - 1, j] = result(columns(chunks * x + j, wide))
                    else:
                        j = int(step[2])
                        fcopy(k, j).wait_recv()
                        gsend[k - 1, j] = (
                            keep[k - 1, j] + frecv[k - 1, j].astype(jnp.float32)
                        ).astype(jnp.bfloat16)
                        gcopy(k, j, c).start()

        @pl.when(inner)
        def _():
            run(INNER, {"N": 3, "F": 2}, True)

        @pl.when(jnp.logical_not(inner))
        def _():
            run(OUTER, {"N": 2, "F": 3}, False)

        pcopy().wait_recv()
        total = own_keep[x] + erecv[x].astype(jnp.float32) + own_recv[...].astype(jnp.float32)
        for k in LAST:
            back = 0.0
            for d in range(2):
                for j in range(part):
                    gcopy(k, j, d).wait_recv()
                returned = jnp.concatenate([grecv[k - 1, d, j] for j in range(part)], axis=1)
                back = back + dot32(place[k - 1, d], returned)
            total = total + back * weight_ref[:, k:k + 1]
        out_ref[...] = total.astype(out_ref.dtype)

        for i in range(3):
            weight_copy(i).wait_send()
        ecopy().wait_send()
        pcopy().wait_send()
        for j in range(redundant):
            rcopy(j).wait_send()
        for k in (1, 2, 3):
            for j in range(chunks):
                zcopy(k, j).wait_send()
                if not redundant_at(k, j):
                    xcopy(k, j).wait_send()
                fcopy(k, j).wait_send()
                gcopy(k, j, c).wait_send()

    return kernel


class NoCopy:
    def start(self):
        pass


def first_use(order):
    return [step for step in order if step[0] == "c"][0]


def fused_body(
    tokens, norm_gain, routing, gate_weights,
    expert_gate, expert_up, expert_down, shared_gate, shared_up, shared_down,
):
    rows, width = tokens.shape
    half = 3 * rows * routing.shape[1] // (2 * 4) // 2
    quarter = width // 4
    ffe = expert_gate.shape[2]
    ffs = shared_gate.shape[1]
    bf16, f32 = jnp.bfloat16, jnp.float32
    dma = pltpu.SemaphoreType.DMA
    vmem = pl.BlockSpec(memory_space=pltpu.VMEM)
    hbm = pl.BlockSpec(memory_space=pl.ANY)
    chunks = CHUNKS
    wide = 2 * quarter // chunks
    piece = (3, chunks, half, wide)
    return pl.pallas_call(
        make_kernel(half, REDUNDANT, chunks),
        out_shape=pltpu.VMEM((rows, quarter), bf16),
        in_specs=[vmem] * 4 + [hbm] * 6,
        out_specs=vmem,
        scratch_shapes=[
            pltpu.VMEM((2, width, ffe), bf16),
            pltpu.VMEM((2, width, ffe), bf16),
            pltpu.VMEM((2, ffe, width), bf16),
            pltpu.VMEM((width, ffs), bf16),
            pltpu.VMEM((width, ffs), bf16),
            pltpu.VMEM((ffs, width), bf16),
            pltpu.VMEM((rows, width), bf16),
            pltpu.VMEM((3, 2, half, rows), bf16),
            pltpu.VMEM((3, 2, rows, half), bf16),
            pltpu.VMEM((rows, 16), f32),
            pltpu.VMEM(piece, bf16),
            pltpu.VMEM((max(REDUNDANT, 1), half, wide), bf16),
            pltpu.VMEM((3, 2 * chunks, half, wide), bf16),
            pltpu.VMEM((2, rows, quarter), bf16),
            pltpu.VMEM((2, rows, quarter), bf16),
            pltpu.VMEM((2, rows, quarter), f32),
            pltpu.VMEM((rows, quarter), bf16),
            pltpu.VMEM((rows, quarter), bf16),
            pltpu.VMEM(piece, bf16),
            pltpu.VMEM(piece, bf16),
            pltpu.VMEM(piece, f32),
            pltpu.VMEM(piece, bf16),
            pltpu.VMEM((3, 2, chunks // 2, half, wide), bf16),
            dma((6,)), pltpu.SemaphoreType.REGULAR((2,)), dma((3,)), dma((3,)),
            dma((3, chunks)), dma((3, chunks)), dma((chunks,)), dma((chunks,)),
            dma((3, chunks)), dma((3, chunks)),
            dma((1,)), dma((1,)), dma((1,)), dma((1,)),
            dma((3, chunks)), dma((3, chunks)), dma((3, chunks)), dma((3, 2, chunks // 2)),
        ],
        compiler_params=pltpu.CompilerParams(collective_id=0, has_side_effects=True),
    )(
        tokens, norm_gain.reshape(1, width), routing.T, gate_weights.T,
        expert_gate[0], expert_up[0], expert_down[0], shared_gate, shared_up, shared_down,
    )


def solution(mesh):
    in_specs = (
        P(("grp", "ep"), None),
        P(),
        P(("grp", "ep"), None),
        P(("grp", "ep"), None),
        P("ep", None, "tp"),
        P("ep", None, "tp"),
        P("ep", "tp", None),
        P(None, "tp"),
        P(None, "tp"),
        P("tp", None),
    )
    out_specs = P(("grp", "ep"), "tp")
    ep_count, tp_count = mesh.shape["ep"], mesh.shape["tp"]

    def layer(*args):
        slots = 3 * args[0].shape[0] * args[2].shape[1] // (8 * mesh.shape["grp"] * ep_count)
        few = tp_count == 4 and ep_count == 4 and args[4].shape[0] == 4 and slots % 32 == 0
        chosen = fused_body if few else body
        return jax.shard_map(
            chosen, mesh=mesh, in_specs=in_specs, out_specs=out_specs, check_vma=False
        )(*args)

    return layer
```
